32 devices in a mesh: sp: 8 (over z, x), dp: 4 (over y, core).
Axes of the slice: x: 2, y: 2, z: 4, core: 2. Of those that a mesh axis runs over, the one named last changes fastest.
Arguments:
- activations: bfloat16 [4, 4096, 2048], P('dp', 'sp'), may hold values from -6 to 6
- value_weight: bfloat16 [2048, 1024], P(('sp', 'dp')), may hold values from -0.125 to 0.125
- gate_weight: bfloat16 [2048, 1024], P(('sp', 'dp')), may hold values from -0.125 to 0.125
- input_weight: bfloat16 [2048, 512], P(('sp', 'dp')), may hold values from -0.125 to 0.125
- readout_weight: bfloat16 [2048, 512], P(('sp', 'dp')), may hold values from -0.125 to 0.125
- rate_weight: bfloat16 [2048, 16], replicated, may hold values from -0.125 to 0.125
- value_taps: bfloat16 [4, 1024], replicated, may hold values from -0.375 to 0.375
- input_taps: bfloat16 [4, 512], replicated, may hold values from -3 to 3
- readout_taps: bfloat16 [4, 512], replicated, may hold values from -3 to 3
- rate_bias: float32 [16], replicated, may hold values from -1 to 1
- decay_log: float32 [16], replicated, may hold values from -1 to 1.5
- norm_gain: float32 [1024], replicated, may hold values from 0.1 to 1.9
- out_weight: bfloat16 [1024, 2048], P(None, ('sp', 'dp')), may hold values from -0.1875 to 0.1875
Outputs:
- mixed_out: bfloat16 [4, 4096, 2048], P('dp', 'sp')
The draws below stay inside these ranges and needn't reach their ends.
All inputs are finite; a program needn't handle non-finite values.
Results may differ from the reference program's by a relative error of at most 0.014.
Values may be sent and summed in bfloat16 or wider, within the bound.
A program may use at most 128 MiB of HBM per device.

```python
import jax
import jax.numpy as jnp
from jax import lax

D = 2048
HEADS = 16
HEAD_DIM = 64
GROUPS = 4
STATE = 128
CONV = 4
BLOCK = 64
WIDTH = 1024
LENGTH = 4096
SEQS = 4


def shard_levels(key, dims, shards, least, high):
    factor_of = 1.0
    for dim, blocks in shards:
        steps = jax.random.uniform(jax.random.fold_in(jax.random.fold_in(key, 6), dim), (blocks,), jnp.float32, least / len(shards), high / len(shards))
        factor_of = factor_of * jnp.repeat(jnp.exp(steps), dims[dim] // blocks).reshape((-1,) + (1,) * (len(dims) - 1 - dim))
    return factor_of


def normal_values(rng, shape, scale, reach, shards=(), kind=jnp.bfloat16):
    level = shard_levels(rng, shape, shards, -0.22, 0.18) if shards else 1.0
    entries = jax.random.normal(rng, shape, jnp.float32) * scale * level
    return jnp.minimum(jnp.maximum(entries, -reach), reach).astype(kind)


def setup_inputs(seed: int = 0) -> dict:
    streams_of = jax.random.split(jax.random.key(seed), 14)
    return {
        "activations": normal_values(streams_of[0], (SEQS, LENGTH, D), 1.0, 6.0, ((0, 4), (1, 8))),
        "value_weight": normal_values(streams_of[1], (D, WIDTH), D ** -0.5, 0.125, ((0, 32),)),
        "gate_weight": normal_values(streams_of[2], (D, WIDTH), D ** -0.5, 0.125, ((0, 32),)),
        "input_weight": normal_values(streams_of[3], (D, GROUPS * STATE), D ** -0.5, 0.125, ((0, 32),)),
        "readout_weight": normal_values(streams_of[4], (D, GROUPS * STATE), D ** -0.5, 0.125, ((0, 32),)),
        "rate_weight": normal_values(streams_of[5], (D, HEADS), D ** -0.5, 0.125),
        "value_taps": normal_values(streams_of[6], (CONV, WIDTH), (64 * CONV) ** -0.5, 0.375),
        "input_taps": normal_values(streams_of[7], (CONV, GROUPS * STATE), CONV ** -0.5, 3.0),
        "readout_taps": normal_values(streams_of[8], (CONV, GROUPS * STATE), CONV ** -0.5, 3.0),
        "rate_bias": jnp.clip(jax.random.uniform(streams_of[9], (HEADS,), jnp.float32, -1.0, 1.0), -1.0, 1.0),
        "decay_log": jnp.clip(jax.random.uniform(streams_of[10], (HEADS,), jnp.float32, -1.0, 1.5), -1.0, 1.5),
        "norm_gain": jnp.clip(1.0 + 0.18 * jax.random.normal(streams_of[11], (WIDTH,), jnp.float32), 0.1, 1.9),
        "out_weight": normal_values(streams_of[12], (WIDTH, D), WIDTH ** -0.5, 0.1875, ((1, 32),)),
    }


norm_eps = 1.0

def broaden(matrix, groups, head_count):
    row_count = matrix.shape[0]
    group_width = matrix.shape[1] // groups
    spread = matrix.reshape(row_count, groups, 1, group_width)
    spread = jnp.broadcast_to(spread, (row_count, groups, head_count // groups, group_width))
    return spread.reshape(row_count, head_count * group_width)

def causal_conv(series, kernel):
    extent = kernel.shape[0]
    length = series.shape[0]
    padded = jnp.pad(series.astype(jnp.float32), ((extent - 1, 0), (0, 0)))
    result = jnp.zeros(series.shape, jnp.float32)
    for offset in range(extent):
        result = result + kernel[offset].astype(jnp.float32) * padded[offset:offset + length]
    return result

def state_mix(values, inputs, readouts, rates, decay):
    length, head_count, head_width = values.shape
    blocks = length // BLOCK
    block_values = values.reshape(blocks, BLOCK, head_count, head_width).astype(jnp.float32)
    block_inputs = inputs.reshape(blocks, BLOCK, head_count, -1).astype(jnp.float32)
    block_reads = readouts.reshape(blocks, BLOCK, head_count, -1).astype(jnp.float32)
    block_rates = rates.reshape(blocks, BLOCK, head_count)
    running = jnp.cumsum(block_rates * decay, axis=1)
    by_head = jnp.transpose(running, (0, 2, 1))
    rate_head = jnp.transpose(block_rates, (0, 2, 1))
    causal = jnp.tril(jnp.ones((BLOCK, BLOCK), dtype=bool))
    intervals = by_head[:, :, :, None] - by_head[:, :, None, :]
    fading = jnp.where(causal, jnp.exp(jnp.minimum(intervals, 0.0)), 0.0)
    intersect = jnp.einsum('bthn,bshn->bhts', block_reads, block_inputs)
    scores = (intersect * fading * rate_head[:, :, None, :]).astype(jnp.bfloat16)
    within = jnp.einsum('bhts,bshp->bthp', scores.astype(jnp.float32), block_values)
    tail_fade = jnp.exp(running[:, -1:, :] - running) * block_rates
    weighted = (block_values * tail_fade[:, :, :, None]).astype(jnp.bfloat16)
    states = jnp.einsum('bshp,bshn->bhpn', weighted.astype(jnp.float32), block_inputs)
    totals = jnp.cumsum(running[:, -1, :], axis=0)
    starts = totals - running[:, -1, :]
    earlier = jnp.tril(jnp.ones((blocks, blocks), dtype=bool), -1)
    carried = jnp.where(earlier[:, :, None], jnp.exp(jnp.minimum(starts[:, None, :] - totals[None, :, :], 0.0)), 0.0)
    entering = jnp.einsum('cdh,dhpn->chpn', carried, states, precision=lax.Precision.HIGHEST)
    across = jnp.einsum('bthn,bhpn->bthp', block_reads, entering, precision=lax.Precision.HIGHEST)
    across = across * jnp.exp(running)[:, :, :, None]
    return (within + across).reshape(length, head_count * head_width)

def reference(activations, value_weight, gate_weight, input_weight, readout_weight, rate_weight, value_taps, input_taps, readout_taps, rate_bias, decay_log, norm_gain, out_weight):

    def mixer(sequence):
        length = sequence.shape[0]
        projected = jnp.dot(sequence, value_weight, preferred_element_type=jnp.float32).astype(jnp.bfloat16)
        gate_proj = jnp.dot(sequence, gate_weight, preferred_element_type=jnp.float32).astype(jnp.bfloat16)
        input_proj = jnp.dot(sequence, input_weight, preferred_element_type=jnp.float32).astype(jnp.bfloat16)
        readout_proj = jnp.dot(sequence, readout_weight, preferred_element_type=jnp.float32).astype(jnp.bfloat16)
        rate_raw = jnp.dot(sequence, rate_weight, preferred_element_type=jnp.float32).astype(jnp.bfloat16)
        conv_values = jax.nn.silu(causal_conv(projected, value_taps)).astype(jnp.bfloat16)
        conv_inputs = jax.nn.silu(causal_conv(input_proj, input_taps)).astype(jnp.bfloat16)
        conv_reads = jax.nn.silu(causal_conv(readout_proj, readout_taps)).astype(jnp.bfloat16)
        head_inputs = broaden(conv_inputs, GROUPS, HEADS).reshape(length, HEADS, STATE)
        head_reads = broaden(conv_reads, GROUPS, HEADS).reshape(length, HEADS, STATE)
        rates = jax.nn.softplus(rate_raw.astype(jnp.float32) + rate_bias)
        decay = -jnp.exp(decay_log) / length
        mixed = state_mix(conv_values.reshape(length, HEADS, HEAD_DIM), head_inputs, head_reads, rates, decay).astype(jnp.bfloat16)
        gated = mixed.astype(jnp.float32) * jax.nn.silu(gate_proj.astype(jnp.float32))
        scale = lax.rsqrt(lax.optimization_barrier(jnp.mean(gated * gated, axis=-1, keepdims=True)) + norm_eps)
        normed = (gated * scale * norm_gain).astype(jnp.bfloat16)
        return jnp.dot(normed, out_weight, preferred_element_type=jnp.float32).astype(jnp.bfloat16)
    return lax.map(mixer, activations)
```

```python
import jax
import jax.numpy as jnp
from jax import lax
from jax.sharding import PartitionSpec as P

HEADS = 16
HEAD_DIM = 64
GROUPS = 4
STATE = 128
BLOCK = 128


norm_eps = 1.0


def project(rows, weight):
    return jnp.dot(rows, weight, preferred_element_type=jnp.float32).astype(jnp.bfloat16)


def halo_conv(series, kernel, length):
    extent = kernel.shape[0]
    lead = series.shape[0] - length
    padded = series.astype(jnp.float32)
    taps = kernel.astype(jnp.float32)
    result = jnp.zeros((length, series.shape[1]), jnp.float32)
    for offset in range(extent):
        first = lead - extent + 1 + offset
        result = result + taps[offset] * padded[first : first + length]
    return jax.nn.silu(result).astype(jnp.bfloat16)


def exact(equation, left, right):
    return jnp.einsum(equation, left, right, precision=lax.Precision.HIGHEST)


def local_mix(values, inputs, reads, rates, decay):
    length = values.shape[0]
    blocks = length // BLOCK
    share = HEADS // GROUPS
    block_values = values.reshape(blocks, BLOCK, GROUPS, share, HEAD_DIM)
    block_inputs = inputs.reshape(blocks, BLOCK, GROUPS, STATE)
    block_reads = reads.reshape(blocks, BLOCK, GROUPS, STATE)
    block_rates = rates.reshape(blocks, BLOCK, HEADS)
    causal = jnp.tril(jnp.ones((BLOCK, BLOCK), dtype=bool))
    running = exact("ts,bsh->bth", causal.astype(jnp.float32), block_rates * decay)
    by_head = jnp.transpose(running, (0, 2, 1))
    rate_head = jnp.transpose(block_rates, (0, 2, 1))
    intervals = by_head[:, :, :, None] - by_head[:, :, None, :]
    fading = jnp.where(causal, jnp.exp(jnp.minimum(intervals, 0.0)), 0.0)
    fading = fading * rate_head[:, :, None, :]
    intersect = jnp.einsum(
        "btgn,bsgn->bgts", block_reads, block_inputs, preferred_element_type=jnp.float32
    )
    fading = fading.reshape(blocks, GROUPS, share, BLOCK, BLOCK)
    scores = (intersect[:, :, None] * fading).astype(jnp.bfloat16)
    within = jnp.einsum(
        "bgkts,bsgkp->btgkp", scores, block_values, preferred_element_type=jnp.float32
    )
    tail_fade = jnp.exp(running[:, -1:, :] - running) * block_rates
    tail_fade = tail_fade.reshape(blocks, BLOCK, GROUPS, share)
    weighted = (block_values.astype(jnp.float32) * tail_fade[..., None]).astype(jnp.bfloat16)
    states = jnp.einsum(
        "bsgkp,bsgn->bgkpn", weighted, block_inputs, preferred_element_type=jnp.float32
    )
    return within, states, running, block_reads


def entering_states(states, running):
    blocks = states.shape[0]
    share = HEADS // GROUPS
    ends = running[:, -1, :]
    totals = jnp.cumsum(ends, axis=0)
    starts = totals - ends
    left = jnp.exp(totals[-1][None] - totals).reshape(blocks, GROUPS, share)
    last = jnp.sum(left[..., None, None] * states, axis=0)
    devices = lax.axis_size("sp")
    mine = lax.axis_index("sp")
    gathered = lax.all_gather(last.astype(jnp.bfloat16), "sp")
    device_ends = lax.all_gather(totals[-1], "sp")
    device_totals = jnp.cumsum(device_ends, axis=0)
    mine_start = device_totals[mine] - device_ends[mine]
    reach = jnp.exp(jnp.minimum(mine_start[None] - device_totals, 0.0))
    reach = jnp.where((jnp.arange(devices) < mine)[:, None], reach, 0.0)
    reach = reach.reshape(devices, GROUPS, share)
    initial = jnp.sum(reach[..., None, None] * gathered.astype(jnp.float32), axis=0)
    current = initial
    entering = []
    for block in range(blocks):
        entering.append(current)
        fade = jnp.exp(ends[block]).reshape(GROUPS, share, 1, 1)
        current = current * fade + states[block]
    return jnp.stack(entering)


def per_device(
    activations,
    value_weight,
    gate_weight,
    input_weight,
    readout_weight,
    rate_weight,
    value_taps,
    input_taps,
    readout_taps,
    rate_bias,
    decay_log,
    norm_gain,
    out_weight,
):
    sequence = activations[0]
    length = sequence.shape[0]
    devices = lax.axis_size("sp")
    halo = lax.ppermute(sequence[-8:], "sp", [(i, i + 1) for i in range(devices - 1)])
    extended = jnp.concatenate([halo, sequence], axis=0)

    def gathered(weight):
        return lax.all_gather(weight, ("sp", "dp"), axis=0, tiled=True)

    value_full = gathered(value_weight)
    input_full = gathered(input_weight)
    readout_full = gathered(readout_weight)
    gate_full = gathered(gate_weight)
    out_full = gathered(out_weight.T)
    rate_raw = project(sequence, rate_weight)
    rates = jax.nn.softplus(rate_raw.astype(jnp.float32) + rate_bias)
    decay = -jnp.exp(decay_log) / (length * devices)
    values = halo_conv(project(extended, value_full), value_taps, length)
    inputs = halo_conv(project(extended, input_full), input_taps, length)
    reads = halo_conv(project(extended, readout_full), readout_taps, length)
    within, states, running, block_reads = local_mix(values, inputs, reads, rates, decay)
    entering = entering_states(states, running).astype(jnp.bfloat16)
    across = jnp.einsum(
        "btgn,bgkpn->btgkp", block_reads, entering, preferred_element_type=jnp.float32
    )
    fade = jnp.exp(running).reshape(across.shape[:4])
    mixed = (within + across * fade[..., None]).reshape(length, HEADS * HEAD_DIM)
    mixed = mixed.astype(jnp.bfloat16)
    gate_proj = project(sequence, gate_full)
    gated = mixed.astype(jnp.float32) * jax.nn.silu(gate_proj.astype(jnp.float32))
    scale = lax.rsqrt(jnp.mean(gated * gated, axis=-1, keepdims=True) + norm_eps)
    normed = (gated * scale * norm_gain).astype(jnp.bfloat16)
    result = lax.dot_general(
        normed, out_full, (((1,), (1,)), ((), ())), preferred_element_type=jnp.float32
    )
    return result.astype(jnp.bfloat16)[None]


def solution(mesh):
    placed = (
        P("dp", "sp", None),
        P(("sp", "dp"), None),
        P(("sp", "dp"), None),
        P(("sp", "dp"), None),
        P(("sp", "dp"), None),
        P(),
        P(),
        P(),
        P(),
        P(),
        P(),
        P(),
        P(None, ("sp", "dp")),
    )
    return jax.shard_map(
        per_device, mesh=mesh, in_specs=placed, out_specs=P("dp", "sp", None), check_vma=False
    )
```

```python
import functools
import itertools

import jax
import jax.numpy as jnp
from jax import lax
from jax.experimental import pallas as pl
from jax.experimental.pallas import tpu as pltpu
from jax.sharding import PartitionSpec as P

HEADS = 16
HEAD_DIM = 64
GROUPS = 4
STATE = 128
BLOCK = 128


norm_eps = 1.0


def nearest(count, place, rank):
    found = 0
    for start in range(count):
        order = sorted(range(count), key=lambda other: (abs(other - start), other))
        found = found + jnp.where(place == start, order[rank], 0)
    return found


def onward(count, place, origin, rank):
    if count == 2:
        return [(1 - place, None)] if rank == 0 else []
    steps = [1, -1] if rank == 0 else [jnp.where(origin < place, 1, -1)]
    pairs = []
    for step in steps:
        target = place + step
        pairs.append((target, jnp.logical_and(target >= 0, target < count)))
    return [pair for pair in pairs if count > 1]


def when(exists, action):
    if exists is None:
        action()
    else:
        pl.when(exists)(action)


def gather_kernel(lines, own_ref, full_ref, send_sem, recv_sem, pair_sem, local_sem):
    depth, across, along, cores = lines
    sp = lax.axis_index("sp")
    dp = lax.axis_index("dp")
    here = (sp // across, sp % across, dp // cores)
    core = dp % cores
    counts = (depth, across, along)

    def target_id(place, which):
        return {"sp": place[0] * across + place[1], "dp": place[2] * cores + which}

    def moved(dim, value):
        return tuple(value if d == dim else here[d] for d in range(3))

    barrier = pltpu.get_barrier_semaphore()
    for dim in range(3):
        for target, exists in onward(counts[dim], here[dim], here[dim], 0):

            def greet(dim=dim, target=target):
                pl.semaphore_signal(
                    barrier,
                    inc=1,
                    device_id=target_id(moved(dim, target), core),
                    device_id_type=pl.DeviceIdType.MESH,
                )

            when(exists, greet)
    pl.semaphore_signal(
        barrier,
        inc=1,
        device_id=target_id(here, 1 - core),
        device_id_type=pl.DeviceIdType.MESH,
    )
    peers = 1
    for dim in range(3):
        for target, exists in onward(counts[dim], here[dim], here[dim], 0):
            peers = peers + (1 if exists is None else jnp.where(exists, 1, 0))
    pl.semaphore_wait(barrier, peers)

    def chip_of(place):
        return (place[0] * across + place[1]) * along + place[2]

    mine = chip_of(here) * cores + core
    local = pltpu.make_async_copy(own_ref, full_ref.at[mine], local_sem)
    local.start()
    ranks = sorted(itertools.product(*(range(n) for n in counts)), key=lambda r: (sum(r), r))
    used = 0
    started = []
    arrivals = []
    for rank in ranks:
        origin = tuple(nearest(counts[d], here[d], rank[d]) for d in range(3))
        chip = chip_of(origin)
        block = chip * cores + core
        for half in range(2):
            landed = full_ref.at[block, half]
            source = own_ref.at[half] if sum(rank) == 0 else landed
            if sum(rank):
                pltpu.make_async_remote_copy(
                    src_ref=landed,
                    dst_ref=landed,
                    send_sem=send_sem.at[0],
                    recv_sem=recv_sem.at[chip, half],
                    device_id=target_id(here, 1 - core),
                    device_id_type=pl.DeviceIdType.MESH,
                ).wait_recv()
            order = (0, 1, 2) if half == 0 else (0, 2, 1)
            hops = []
            for position in (2, 1, 0):
                if any(rank[order[later]] for later in range(position + 1, 3)):
                    continue
                dim = order[position]
                for target, exists in onward(counts[dim], here[dim], origin[dim], rank[dim]):
                    hops.append((target_id(moved(dim, target), core), recv_sem, exists))
            hops.append((target_id(here, 1 - core), pair_sem, None))
            for device, sem, exists in hops:
                copy = pltpu.make_async_remote_copy(
                    src_ref=source,
                    dst_ref=landed,
                    send_sem=send_sem.at[used],
                    recv_sem=sem.at[chip, half],
                    device_id=device,
                    device_id_type=pl.DeviceIdType.MESH,
                )
                used += 1
                when(exists, copy.start)
                started.append((copy, exists))
    for copy, exists in started:
        when(exists, copy.wait_send)
    for chip in range(depth * across * along):
        for half in range(2):
            landed = full_ref.at[chip * cores + 1 - core, half]
            pltpu.make_async_remote_copy(
                src_ref=landed,
                dst_ref=landed,
                send_sem=send_sem.at[0],
                recv_sem=pair_sem.at[chip, half],
                device_id=target_id(here, 1 - core),
                device_id_type=pl.DeviceIdType.MESH,
            ).wait_recv()
    local.wait()


def gather_rows(own):
    sp, dp = lax.axis_size("sp"), lax.axis_size("dp")
    across = 1
    while 4 * across * across <= sp:
        across *= 2
    lines = (sp // across, across, dp // 2, 2)
    chips = sp * dp // 2
    rows, columns = own.shape
    hops = 2 * chips * 7
    full = pl.pallas_call(
        functools.partial(gather_kernel, lines),
        out_shape=jax.ShapeDtypeStruct((sp * dp, 2, rows // 2, columns), own.dtype),
        in_specs=[pl.BlockSpec(memory_space=pltpu.VMEM)],
        out_specs=pl.BlockSpec(memory_space=pl.ANY),
        scratch_shapes=[
            pltpu.SemaphoreType.DMA((hops,)),
            pltpu.SemaphoreType.DMA((chips, 2)),
            pltpu.SemaphoreType.DMA((chips, 2)),
            pltpu.SemaphoreType.DMA,
        ],
        compiler_params=pltpu.CompilerParams(collective_id=1, has_side_effects=True),
    )(own.reshape(2, rows // 2, columns))
    return full.reshape(sp * dp * rows, columns)


def project(rows, weight):
    return jnp.dot(rows, weight, preferred_element_type=jnp.float32).astype(jnp.bfloat16)


def halo_conv(series, kernel, length):
    extent = kernel.shape[0]
    lead = series.shape[0] - length
    padded = series.astype(jnp.float32)
    taps = kernel.astype(jnp.float32)
    result = jnp.zeros((length, series.shape[1]), jnp.float32)
    for offset in range(extent):
        first = lead - extent + 1 + offset
        result = result + taps[offset] * padded[first : first + length]
    return jax.nn.silu(result).astype(jnp.bfloat16)


def exact(equation, left, right):
    return jnp.einsum(equation, left, right, precision=lax.Precision.HIGHEST)


def local_mix(values, inputs, reads, rates, decay):
    length = values.shape[0]
    blocks = length // BLOCK
    share = HEADS // GROUPS
    block_values = values.reshape(blocks, BLOCK, GROUPS, share, HEAD_DIM)
    block_inputs = inputs.reshape(blocks, BLOCK, GROUPS, STATE)
    block_reads = reads.reshape(blocks, BLOCK, GROUPS, STATE)
    block_rates = rates.reshape(blocks, BLOCK, HEADS)
    causal = jnp.tril(jnp.ones((BLOCK, BLOCK), dtype=bool))
    running = exact("ts,bsh->bth", causal.astype(jnp.float32), block_rates * decay)
    by_head = jnp.transpose(running, (0, 2, 1))
    rate_head = jnp.transpose(block_rates, (0, 2, 1))
    intervals = by_head[:, :, :, None] - by_head[:, :, None, :]
    fading = jnp.where(causal, jnp.exp(jnp.minimum(intervals, 0.0)), 0.0)
    fading = fading * rate_head[:, :, None, :]
    intersect = jnp.einsum(
        "btgn,bsgn->bgts", block_reads, block_inputs, preferred_element_type=jnp.float32
    )
    fading = fading.reshape(blocks, GROUPS, share, BLOCK, BLOCK)
    scores = (intersect[:, :, None] * fading).astype(jnp.bfloat16)
    within = jnp.einsum(
        "bgkts,bsgkp->btgkp", scores, block_values, preferred_element_type=jnp.float32
    )
    tail_fade = jnp.exp(running[:, -1:, :] - running) * block_rates
    tail_fade = tail_fade.reshape(blocks, BLOCK, GROUPS, share)
    weighted = (block_values.astype(jnp.float32) * tail_fade[..., None]).astype(jnp.bfloat16)
    states = jnp.einsum(
        "bsgkp,bsgn->bgkpn", weighted, block_inputs, preferred_element_type=jnp.float32
    )
    return within, states, running, block_reads


def entering_states(states, running):
    blocks = states.shape[0]
    share = HEADS // GROUPS
    ends = running[:, -1, :]
    totals = jnp.cumsum(ends, axis=0)
    starts = totals - ends
    left = jnp.exp(totals[-1][None] - totals).reshape(blocks, GROUPS, share)
    last = jnp.sum(left[..., None, None] * states, axis=0)
    devices = lax.axis_size("sp")
    held = last
    span = totals[-1]
    stride = 1
    while stride < devices:
        pairs = [(i, i + stride) for i in range(devices - stride)]
        came = lax.ppermute(held.astype(jnp.bfloat16), "sp", pairs).astype(jnp.float32)
        held = held + jnp.exp(span).reshape(GROUPS, share, 1, 1) * came
        span = span + lax.ppermute(span, "sp", pairs)
        stride *= 2
    pairs = [(i, i + 1) for i in range(devices - 1)]
    initial = lax.ppermute(held.astype(jnp.bfloat16), "sp", pairs).astype(jnp.float32)
    current = initial
    entering = []
    for block in range(blocks):
        entering.append(current)
        fade = jnp.exp(ends[block]).reshape(GROUPS, share, 1, 1)
        current = current * fade + states[block]
    return jnp.stack(entering)


def per_device(
    activations,
    value_weight,
    gate_weight,
    input_weight,
    readout_weight,
    rate_weight,
    value_taps,
    input_taps,
    readout_taps,
    rate_bias,
    decay_log,
    norm_gain,
    out_weight,
):
    sequence = activations[0]
    length = sequence.shape[0]
    devices = lax.axis_size("sp")
    halo = lax.ppermute(sequence[-8:], "sp", [(i, i + 1) for i in range(devices - 1)])
    extended = jnp.concatenate([halo, sequence], axis=0)

    own = jnp.concatenate(
        [value_weight, input_weight, readout_weight, gate_weight, out_weight.T], axis=1
    )
    full = gather_rows(own)
    ends = [0]
    for weight in (value_weight, input_weight, readout_weight, gate_weight):
        ends.append(ends[-1] + weight.shape[1])
    rate_raw = project(sequence, rate_weight)
    rates = jax.nn.softplus(rate_raw.astype(jnp.float32) + rate_bias)
    decay = -jnp.exp(decay_log) / (length * devices)
    projected = project(extended, full[:, : ends[4]])
    values = halo_conv(projected[:, ends[0] : ends[1]], value_taps, length)
    inputs = halo_conv(projected[:, ends[1] : ends[2]], input_taps, length)
    reads = halo_conv(projected[:, ends[2] : ends[3]], readout_taps, length)
    within, states, running, block_reads = local_mix(values, inputs, reads, rates, decay)
    entering = entering_states(states, running).astype(jnp.bfloat16)
    across = jnp.einsum(
        "btgn,bgkpn->btgkp", block_reads, entering, preferred_element_type=jnp.float32
    )
    fade = jnp.exp(running).reshape(across.shape[:4])
    mixed = (within + across * fade[..., None]).reshape(length, HEADS * HEAD_DIM)
    mixed = mixed.astype(jnp.bfloat16)
    gate_proj = projected[halo.shape[0] :, ends[3] : ends[4]]
    gated = mixed.astype(jnp.float32) * jax.nn.silu(gate_proj.astype(jnp.float32))
    scale = lax.rsqrt(jnp.mean(gated * gated, axis=-1, keepdims=True) + norm_eps)
    normed = (gated * scale * norm_gain).astype(jnp.bfloat16)
    result = lax.dot_general(
        normed, full[:, ends[4] :], (((1,), (1,)), ((), ())), preferred_element_type=jnp.float32
    )
    return result.astype(jnp.bfloat16)[None]


def solution(mesh):
    placed = (
        P("dp", "sp", None),
        P(("sp", "dp"), None),
        P(("sp", "dp"), None),
        P(("sp", "dp"), None),
        P(("sp", "dp"), None),
        P(),
        P(),
        P(),
        P(),
        P(),
        P(),
        P(),
        P(None, ("sp", "dp")),
    )
    return jax.shard_map(
        per_device, mesh=mesh, in_specs=placed, out_specs=P("dp", "sp", None), check_vma=False
    )
```

```python
import functools
import itertools

import jax
import jax.numpy as jnp
from jax import lax
from jax.experimental import pallas as pl
from jax.experimental.pallas import tpu as pltpu
from jax.sharding import PartitionSpec as P

HEADS = 16
HEAD_DIM = 64
GROUPS = 4
STATE = 128
BLOCK = 128


norm_eps = 1.0


def nearest(count, place, rank):
    found = 0
    for start in range(count):
        order = sorted(range(count), key=lambda other: (abs(other - start), other))
        found = found + jnp.where(place == start, order[rank], 0)
    return found


def onward(count, place, origin, rank):
    if count == 2:
        return [(1 - place, None)] if rank == 0 else []
    steps = [1, -1] if rank == 0 else [jnp.where(origin < place, 1, -1)]
    pairs = []
    for step in steps:
        target = place + step
        pairs.append((target, jnp.logical_and(target >= 0, target < count)))
    return [pair for pair in pairs if count > 1]


def when(exists, action):
    if exists is None:
        action()
    else:
        pl.when(exists)(action)


def gather_kernel(
    lines,
    own_ref,
    tail_ref,
    span_ref,
    full_ref,
    halo_ref,
    spans_ref,
    send_sem,
    recv_sem,
    pair_sem,
    local_sem,
    halo_sem,
    span_send,
    span_recv,
):
    depth, across, along, cores = lines
    sp = lax.axis_index("sp")
    dp = lax.axis_index("dp")
    here = (sp // across, sp % across, dp // cores)
    core = dp % cores
    counts = (depth, across, along)

    def target_id(place, which):
        return {"sp": place[0] * across + place[1], "dp": place[2] * cores + which}

    def moved(dim, value):
        return tuple(value if d == dim else here[d] for d in range(3))

    barrier = pltpu.get_barrier_semaphore()
    devices = depth * across
    peers = devices
    for step in range(1, devices):
        pl.semaphore_signal(
            barrier,
            inc=1,
            device_id={"sp": (sp + step) % devices, "dp": dp},
            device_id_type=pl.DeviceIdType.MESH,
        )
    for target, exists in onward(along, here[2], here[2], 0):

        def greet(target=target):
            pl.semaphore_signal(
                barrier,
                inc=1,
                device_id=target_id(moved(2, target), core),
                device_id_type=pl.DeviceIdType.MESH,
            )

        when(exists, greet)
        peers = peers + (1 if exists is None else jnp.where(exists, 1, 0))
    pl.semaphore_signal(
        barrier,
        inc=1,
        device_id=target_id(here, 1 - core),
        device_id_type=pl.DeviceIdType.MESH,
    )
    pl.semaphore_wait(barrier, peers)

    halo_copy = pltpu.make_async_remote_copy(
        src_ref=tail_ref,
        dst_ref=halo_ref,
        send_sem=halo_sem.at[0],
        recv_sem=halo_sem.at[1],
        device_id={"sp": (sp + 1) % devices, "dp": dp},
        device_id_type=pl.DeviceIdType.MESH,
    )
    pl.when(sp + 1 < devices)(halo_copy.start)
    own_span = pltpu.make_async_copy(span_ref, spans_ref.at[sp], halo_sem.at[2])
    own_span.start()

    def span_copy(step, slot):
        return pltpu.make_async_remote_copy(
            src_ref=span_ref,
            dst_ref=spans_ref.at[slot],
            send_sem=span_send.at[step - 1],
            recv_sem=span_recv.at[step - 1],
            device_id={"sp": (sp + step) % devices, "dp": dp},
            device_id_type=pl.DeviceIdType.MESH,
        )

    for step in range(1, devices):
        span_copy(step, sp).start()

    def chip_of(place):
        return (place[0] * across + place[1]) * along + place[2]

    mine = chip_of(here) * cores + core
    local = pltpu.make_async_copy(own_ref, full_ref.at[mine], local_sem)
    local.start()
    ranks = sorted(itertools.product(*(range(n) for n in counts)), key=lambda r: (sum(r), r))
    used = 0
    started = []
    arrivals = []
    for rank in ranks:
        origin = tuple(nearest(counts[d], here[d], rank[d]) for d in range(3))
        chip = chip_of(origin)
        block = chip * cores + core
        for half in range(2):
            landed = full_ref.at[block, half]
            source = own_ref.at[half] if sum(rank) == 0 else landed
            if sum(rank):
                pltpu.make_async_remote_copy(
                    src_ref=landed,
                    dst_ref=landed,
                    send_sem=send_sem.at[0],
                    recv_sem=recv_sem.at[chip, half],
                    device_id=target_id(here, 1 - core),
                    device_id_type=pl.DeviceIdType.MESH,
                ).wait_recv()
            order = (0, 1, 2) if half == 0 else (0, 2, 1)
            hops = []
            for position in (2, 1, 0):
                if any(rank[order[later]] for later in range(position + 1, 3)):
                    continue
                dim = order[position]
                for target, exists in onward(counts[dim], here[dim], origin[dim], rank[dim]):
                    hops.append((target_id(moved(dim, target), core), recv_sem, exists))
            hops.append((target_id(here, 1 - core), pair_sem, None))
            for device, sem, exists in hops:
                copy = pltpu.make_async_remote_copy(
                    src_ref=source,
                    dst_ref=landed,
                    send_sem=send_sem.at[used],
                    recv_sem=sem.at[chip, half],
                    device_id=device,
                    device_id_type=pl.DeviceIdType.MESH,
                )
                used += 1
                when(exists, copy.start)
                started.append((copy, exists))
    for copy, exists in started:
        when(exists, copy.wait_send)
    for chip in range(depth * across * along):
        for half in range(2):
            landed = full_ref.at[chip * cores + 1 - core, half]
            pltpu.make_async_remote_copy(
                src_ref=landed,
                dst_ref=landed,
                send_sem=send_sem.at[0],
                recv_sem=pair_sem.at[chip, half],
                device_id=target_id(here, 1 - core),
                device_id_type=pl.DeviceIdType.MESH,
            ).wait_recv()
    local.wait()
    own_span.wait()
    for step in range(1, devices):
        span_copy(step, sp).wait_send()
        span_copy(step, (sp + devices - step) % devices).wait_recv()
    pl.when(sp + 1 < devices)(halo_copy.wait_send)
    pl.when(sp > 0)(halo_copy.wait_recv)


def exchange_kernel(devices, in_ref, out_ref, send_sem, recv_sem, local_sem):
    sp = lax.axis_index("sp")
    dp = lax.axis_index("dp")
    barrier = pltpu.get_barrier_semaphore()
    for step in range(1, devices):
        pl.semaphore_signal(
            barrier,
            inc=1,
            device_id={"sp": (sp + step) % devices, "dp": dp},
            device_id_type=pl.DeviceIdType.MESH,
        )
    pl.semaphore_wait(barrier, devices - 1)

    def copy(step, slot):
        target = (sp + step) % devices
        return pltpu.make_async_remote_copy(
            src_ref=in_ref.at[target],
            dst_ref=out_ref.at[slot],
            send_sem=send_sem.at[step - 1],
            recv_sem=recv_sem.at[step - 1],
            device_id={"sp": target, "dp": dp},
            device_id_type=pl.DeviceIdType.MESH,
        )

    for step in range(1, devices):
        copy(step, sp).start()
    local = pltpu.make_async_copy(in_ref.at[sp], out_ref.at[sp], local_sem)
    local.start()
    for step in range(1, devices):
        copy(step, sp).wait_send()
        copy(step, (sp + devices - step) % devices).wait_recv()
    local.wait()


def exchange(blocks, identity):
    devices = blocks.shape[0]
    return pl.pallas_call(
        functools.partial(exchange_kernel, devices),
        out_shape=jax.ShapeDtypeStruct(blocks.shape, blocks.dtype),
        in_specs=[pl.BlockSpec(memory_space=pltpu.VMEM)],
        out_specs=pl.BlockSpec(memory_space=pltpu.VMEM),
        scratch_shapes=[
            pltpu.SemaphoreType.DMA((devices - 1,)),
            pltpu.SemaphoreType.DMA((devices - 1,)),
            pltpu.SemaphoreType.DMA,
        ],
        compiler_params=pltpu.CompilerParams(collective_id=identity, has_side_effects=True),
    )(blocks)


def gather_rows(own, tail, span):
    sp, dp = lax.axis_size("sp"), lax.axis_size("dp")
    across = 1
    while 4 * across * across <= sp:
        across *= 2
    lines = (sp // across, across, dp // 2, 2)
    chips = sp * dp // 2
    rows, columns = own.shape
    hops = 2 * chips * 7
    full, halo, spans = pl.pallas_call(
        functools.partial(gather_kernel, lines),
        out_shape=(
            jax.ShapeDtypeStruct((sp * dp, 2, rows // 2, columns), own.dtype),
            jax.ShapeDtypeStruct(tail.shape, tail.dtype),
            jax.ShapeDtypeStruct((sp,) + span.shape, span.dtype),
        ),
        in_specs=[pl.BlockSpec(memory_space=pltpu.VMEM)] * 3,
        out_specs=(
            pl.BlockSpec(memory_space=pl.ANY),
            pl.BlockSpec(memory_space=pltpu.VMEM),
            pl.BlockSpec(memory_space=pltpu.VMEM),
        ),
        scratch_shapes=[
            pltpu.SemaphoreType.DMA((hops,)),
            pltpu.SemaphoreType.DMA((chips, 2)),
            pltpu.SemaphoreType.DMA((chips, 2)),
            pltpu.SemaphoreType.DMA,
            pltpu.SemaphoreType.DMA((3,)),
            pltpu.SemaphoreType.DMA((sp - 1,)),
            pltpu.SemaphoreType.DMA((sp - 1,)),
        ],
        compiler_params=pltpu.CompilerParams(collective_id=1, has_side_effects=True),
    )(own.reshape(2, rows // 2, columns), tail, span)
    return full.reshape(sp * dp * rows, columns), halo, spans


def project(rows, weight):
    return jnp.dot(rows, weight, preferred_element_type=jnp.float32).astype(jnp.bfloat16)


def halo_conv(series, kernel, length):
    extent = kernel.shape[0]
    lead = series.shape[0] - length
    padded = series.astype(jnp.float32)
    taps = kernel.astype(jnp.float32)
    result = jnp.zeros((length, series.shape[1]), jnp.float32)
    for offset in range(extent):
        first = lead - extent + 1 + offset
        result = result + taps[offset] * padded[first : first + length]
    return jax.nn.silu(result).astype(jnp.bfloat16)


def exact(equation, left, right):
    return jnp.einsum(equation, left, right, precision=lax.Precision.HIGHEST)


def local_mix(values, inputs, reads, rates, decay):
    length = values.shape[0]
    blocks = length // BLOCK
    share = HEADS // GROUPS
    block_values = values.reshape(blocks, BLOCK, GROUPS, share, HEAD_DIM)
    block_inputs = inputs.reshape(blocks, BLOCK, GROUPS, STATE)
    block_reads = reads.reshape(blocks, BLOCK, GROUPS, STATE)
    block_rates = rates.reshape(blocks, BLOCK, HEADS)
    causal = jnp.tril(jnp.ones((BLOCK, BLOCK), dtype=bool))
    running = exact("ts,bsh->bth", causal.astype(jnp.float32), block_rates * decay)
    by_head = jnp.transpose(running, (0, 2, 1))
    rate_head = jnp.transpose(block_rates, (0, 2, 1))
    intervals = by_head[:, :, :, None] - by_head[:, :, None, :]
    fading = jnp.where(causal, jnp.exp(jnp.minimum(intervals, 0.0)), 0.0)
    fading = fading * rate_head[:, :, None, :]
    intersect = jnp.einsum(
        "btgn,bsgn->bgts", block_reads, block_inputs, preferred_element_type=jnp.float32
    )
    fading = fading.reshape(blocks, GROUPS, share, BLOCK, BLOCK)
    scores = (intersect[:, :, None] * fading).astype(jnp.bfloat16)
    within = jnp.einsum(
        "bgkts,bsgkp->btgkp", scores, block_values, preferred_element_type=jnp.float32
    )
    tail_fade = jnp.exp(running[:, -1:, :] - running) * block_rates
    tail_fade = tail_fade.reshape(blocks, BLOCK, GROUPS, share)
    weighted = (block_values.astype(jnp.float32) * tail_fade[..., None]).astype(jnp.bfloat16)
    states = jnp.einsum(
        "bsgkp,bsgn->bgkpn", weighted, block_inputs, preferred_element_type=jnp.float32
    )
    return within, states, running, block_reads


def entering_states(states, running, spans):
    blocks = states.shape[0]
    share = HEADS // GROUPS
    ends = running[:, -1, :]
    totals = jnp.cumsum(ends, axis=0)
    starts = totals - ends
    left = jnp.exp(totals[-1][None] - totals).reshape(blocks, GROUPS, share)
    last = jnp.sum(left[..., None, None] * states, axis=0)
    devices = lax.axis_size("sp")
    held = HEADS // devices
    came = exchange(last.astype(jnp.bfloat16).reshape(devices, held, HEAD_DIM, STATE), 2)
    own_spans = lax.dynamic_slice_in_dim(spans, lax.axis_index("sp") * held, held, 1)
    fades = jnp.exp(own_spans)[:, :, None, None]
    reached = jnp.zeros(came.shape[1:], jnp.float32)
    leaving = []
    for device in range(devices):
        leaving.append(reached.astype(jnp.bfloat16))
        reached = reached * fades[device] + came[device].astype(jnp.float32)
    initial = exchange(jnp.stack(leaving), 3).astype(jnp.float32)
    initial = initial.reshape(GROUPS, share, HEAD_DIM, STATE)
    current = initial
    entering = []
    for block in range(blocks):
        entering.append(current)
        fade = jnp.exp(ends[block]).reshape(GROUPS, share, 1, 1)
        current = current * fade + states[block]
    return jnp.stack(entering)


def per_device(
    activations,
    value_weight,
    gate_weight,
    input_weight,
    readout_weight,
    rate_weight,
    value_taps,
    input_taps,
    readout_taps,
    rate_bias,
    decay_log,
    norm_gain,
    out_weight,
):
    sequence = activations[0]
    length = sequence.shape[0]
    devices = lax.axis_size("sp")

    own = jnp.concatenate(
        [value_weight, input_weight, readout_weight, gate_weight, out_weight.T], axis=1
    )
    rate_raw = project(sequence, rate_weight)
    rates = jax.nn.softplus(rate_raw.astype(jnp.float32) + rate_bias)
    decay = -jnp.exp(decay_log) / (length * devices)
    span = jnp.zeros((8, 128), jnp.float32).at[:, :HEADS].set(jnp.sum(rates * decay, axis=0))
    full, halo, spans = gather_rows(own, sequence[-8:], span)
    spans = spans[:, 0, :HEADS]
    halo = jnp.where(lax.axis_index("sp") > 0, halo, jnp.zeros_like(halo))
    extended = jnp.concatenate([halo, sequence], axis=0)
    ends = [0]
    for weight in (value_weight, input_weight, readout_weight, gate_weight):
        ends.append(ends[-1] + weight.shape[1])
    projected = project(extended, full[:, : ends[4]])
    values = halo_conv(projected[:, ends[0] : ends[1]], value_taps, length)
    inputs = halo_conv(projected[:, ends[1] : ends[2]], input_taps, length)
    reads = halo_conv(projected[:, ends[2] : ends[3]], readout_taps, length)
    within, states, running, block_reads = local_mix(values, inputs, reads, rates, decay)
    entering = entering_states(states, running, spans).astype(jnp.bfloat16)
    across = jnp.einsum(
        "btgn,bgkpn->btgkp", block_reads, entering, preferred_element_type=jnp.float32
    )
    fade = jnp.exp(running).reshape(across.shape[:4])
    mixed = (within + across * fade[..., None]).reshape(length, HEADS * HEAD_DIM)
    mixed = mixed.astype(jnp.bfloat16)
    gate_proj = projected[halo.shape[0] :, ends[3] : ends[4]]
    gated = mixed.astype(jnp.float32) * jax.nn.silu(gate_proj.astype(jnp.float32))
    scale = lax.rsqrt(jnp.mean(gated * gated, axis=-1, keepdims=True) + norm_eps)
    normed = (gated * scale * norm_gain).astype(jnp.bfloat16)
    result = lax.dot_general(
        normed, full[:, ends[4] :], (((1,), (1,)), ((), ())), preferred_element_type=jnp.float32
    )
    return result.astype(jnp.bfloat16)[None]


def solution(mesh):
    placed = (
        P("dp", "sp", None),
        P(("sp", "dp"), None),
        P(("sp", "dp"), None),
        P(("sp", "dp"), None),
        P(("sp", "dp"), None),
        P(),
        P(),
        P(),
        P(),
        P(),
        P(),
        P(),
        P(None, ("sp", "dp")),
    )
    return jax.shard_map(
        per_device, mesh=mesh, in_specs=placed, out_specs=P("dp", "sp", None), check_vma=False
    )
```

```python
import functools
import itertools

import jax
import jax.numpy as jnp
from jax import lax
from jax.experimental import pallas as pl
from jax.experimental.pallas import tpu as pltpu
from jax.sharding import PartitionSpec as P

HEADS = 16
HEAD_DIM = 64
GROUPS = 4
STATE = 128
BLOCK = 128
LAG = 2
TILE = 512


norm_eps = 1.0


def nearest(count, place, rank):
    found = 0
    for start in range(count):
        order = sorted(range(count), key=lambda other: (abs(other - start), other))
        found = found + jnp.where(place == start, order[rank], 0)
    return found


def onward(count, place, origin, rank):
    if count == 2:
        return [(1 - place, None)] if rank == 0 else []
    steps = [1, -1] if rank == 0 else [jnp.where(origin < place, 1, -1)]
    pairs = []
    for step in steps:
        target = place + step
        pairs.append((target, jnp.logical_and(target >= 0, target < count)))
    return [pair for pair in pairs if count > 1]


def when(exists, action):
    if exists is None:
        action()
    else:
        pl.when(exists)(action)


def gather_kernel(
    lines,
    own_ref,
    tail_ref,
    span_ref,
    *rest,
):
    fused = len(rest) > 10
    if fused:
        seq_ref, proj_ref, outw_ref, spans_ref = rest[:4]
        full_ref, halo_ref, ext_ref, acc_ref, out_sem = rest[4:9]
    else:
        full_ref, halo_ref, spans_ref = rest[:3]
    (
        send_sem,
        recv_sem,
        pair_sem,
        local_sem,
        halo_sem,
        span_send,
        span_recv,
    ) = rest[-7:]
    depth, across, along, cores = lines
    sp = lax.axis_index("sp")
    dp = lax.axis_index("dp")
    here = (sp // across, sp % across, dp // cores)
    core = dp % cores
    counts = (depth, across, along)

    def target_id(place, which):
        return {"sp": place[0] * across + place[1], "dp": place[2] * cores + which}

    def moved(dim, value):
        return tuple(value if d == dim else here[d] for d in range(3))

    barrier = pltpu.get_barrier_semaphore()
    devices = depth * across
    peers = devices
    for step in range(1, devices):
        pl.semaphore_signal(
            barrier,
            inc=1,
            device_id={"sp": (sp + step) % devices, "dp": dp},
            device_id_type=pl.DeviceIdType.MESH,
        )
    for target, exists in onward(along, here[2], here[2], 0):

        def greet(target=target):
            pl.semaphore_signal(
                barrier,
                inc=1,
                device_id=target_id(moved(2, target), core),
                device_id_type=pl.DeviceIdType.MESH,
            )

        when(exists, greet)
        peers = peers + (1 if exists is None else jnp.where(exists, 1, 0))
    pl.semaphore_signal(
        barrier,
        inc=1,
        device_id=target_id(here, 1 - core),
        device_id_type=pl.DeviceIdType.MESH,
    )
    pl.semaphore_wait(barrier, peers)

    halo_copy = pltpu.make_async_remote_copy(
        src_ref=tail_ref,
        dst_ref=halo_ref,
        send_sem=halo_sem.at[0],
        recv_sem=halo_sem.at[1],
        device_id={"sp": (sp + 1) % devices, "dp": dp},
        device_id_type=pl.DeviceIdType.MESH,
    )
    pl.when(sp + 1 < devices)(halo_copy.start)
    own_span = pltpu.make_async_copy(span_ref, spans_ref.at[sp], halo_sem.at[2])
    own_span.start()

    def span_copy(step, slot):
        return pltpu.make_async_remote_copy(
            src_ref=span_ref,
            dst_ref=spans_ref.at[slot],
            send_sem=span_send.at[step - 1],
            recv_sem=span_recv.at[step - 1],
            device_id={"sp": (sp + step) % devices, "dp": dp},
            device_id_type=pl.DeviceIdType.MESH,
        )

    for step in range(1, devices):
        span_copy(step, sp).start()

    def chip_of(place):
        return (place[0] * across + place[1]) * along + place[2]

    mine = chip_of(here) * cores + core
    local = pltpu.make_async_copy(own_ref, full_ref.at[mine], local_sem)
    local.start()
    ranks = sorted(itertools.product(*(range(n) for n in counts)), key=lambda r: (sum(r), r))
    used = 0
    started = []
    chips = []

    def wait_pair(chip):
        for half in range(2):
            landed = full_ref.at[chip * cores + 1 - core, half]
            pltpu.make_async_remote_copy(
                src_ref=landed,
                dst_ref=landed,
                send_sem=send_sem.at[0],
                recv_sem=pair_sem.at[chip, half],
                device_id=target_id(here, 1 - core),
                device_id_type=pl.DeviceIdType.MESH,
            ).wait_recv()

    def out_copy(chip):
        width = proj_ref.shape[1]
        return pltpu.make_async_copy(
            full_ref.at[pl.ds(chip * cores, cores), :, :, pl.ds(width, outw_ref.shape[3])],
            outw_ref.at[pl.ds(chip * cores, cores)],
            out_sem.at[chip],
        )

    def accumulate(event):
        chip = chips[event]
        if event == 0:
            local.wait()
            lead = halo_ref.shape[0]

            def take():
                halo_copy.wait_recv()
                ext_ref[:lead] = halo_ref[...]

            def clear():
                ext_ref[:lead] = jnp.zeros_like(halo_ref)

            pl.when(sp > 0)(take)
            pl.when(sp == 0)(clear)
        wait_pair(chip)
        out_copy(chip).start()
        depth_rows = cores * 2 * full_ref.shape[2]
        rows = ext_ref[:, pl.ds(pl.multiple_of(chip * depth_rows, 128), depth_rows)]

        def tile(index, carry):
            columns = pl.ds(pl.multiple_of(index * TILE, TILE), TILE)
            piece = full_ref[pl.ds(chip * cores, cores), :, :, columns].reshape(depth_rows, TILE)
            product = jnp.dot(rows, piece, preferred_element_type=jnp.float32)
            if event == 0:
                acc_ref[:, columns] = product
            elif event == len(ranks) - 1:
                proj_ref[:, columns] = (acc_ref[:, columns] + product).astype(proj_ref.dtype)
            else:
                acc_ref[:, columns] += product
            return carry

        lax.fori_loop(0, proj_ref.shape[1] // TILE, tile, 0)

    for rank in ranks:
        origin = tuple(nearest(counts[d], here[d], rank[d]) for d in range(3))
        chip = chip_of(origin)
        block = chip * cores + core
        for half in range(2):
            landed = full_ref.at[block, half]
            source = own_ref.at[half] if sum(rank) == 0 else landed
            if sum(rank):
                pltpu.make_async_remote_copy(
                    src_ref=landed,
                    dst_ref=landed,
                    send_sem=send_sem.at[0],
                    recv_sem=recv_sem.at[chip, half],
                    device_id=target_id(here, 1 - core),
                    device_id_type=pl.DeviceIdType.MESH,
                ).wait_recv()
            order = (0, 1, 2) if half == 0 else (0, 2, 1)
            hops = []
            for position in (2, 1, 0):
                if any(rank[order[later]] for later in range(position + 1, 3)):
                    continue
                dim = order[position]
                for target, exists in onward(counts[dim], here[dim], origin[dim], rank[dim]):
                    hops.append((target_id(moved(dim, target), core), recv_sem, exists))
            hops.append((target_id(here, 1 - core), pair_sem, None))
            for device, sem, exists in hops:
                copy = pltpu.make_async_remote_copy(
                    src_ref=source,
                    dst_ref=landed,
                    send_sem=send_sem.at[used],
                    recv_sem=sem.at[chip, half],
                    device_id=device,
                    device_id_type=pl.DeviceIdType.MESH,
                )
                used += 1
                when(exists, copy.start)
                started.append((copy, exists))
        chips.append(chip)
        if fused and len(chips) == 1:
            ext_ref[halo_ref.shape[0] :] = seq_ref[...]
        if fused and len(chips) > LAG:
            accumulate(len(chips) - 1 - LAG)
    if fused:
        for event in range(len(chips) - LAG, len(chips)):
            accumulate(event)
    for copy, exists in started:
        when(exists, copy.wait_send)
    for chip in range(depth * across * along):
        if fused:
            out_copy(chip).wait()
        else:
            wait_pair(chip)
    if not fused:
        local.wait()
        pl.when(sp > 0)(halo_copy.wait_recv)
    own_span.wait()
    for step in range(1, devices):
        span_copy(step, sp).wait_send()
        span_copy(step, (sp + devices - step) % devices).wait_recv()
    pl.when(sp + 1 < devices)(halo_copy.wait_send)


def exchange_kernel(devices, in_ref, out_ref, send_sem, recv_sem, local_sem):
    sp = lax.axis_index("sp")
    dp = lax.axis_index("dp")
    barrier = pltpu.get_barrier_semaphore()
    for step in range(1, devices):
        pl.semaphore_signal(
            barrier,
            inc=1,
            device_id={"sp": (sp + step) % devices, "dp": dp},
            device_id_type=pl.DeviceIdType.MESH,
        )
    pl.semaphore_wait(barrier, devices - 1)

    def copy(step, slot):
        target = (sp + step) % devices
        return pltpu.make_async_remote_copy(
            src_ref=in_ref.at[target],
            dst_ref=out_ref.at[slot],
            send_sem=send_sem.at[step - 1],
            recv_sem=recv_sem.at[step - 1],
            device_id={"sp": target, "dp": dp},
            device_id_type=pl.DeviceIdType.MESH,
        )

    for step in range(1, devices):
        copy(step, sp).start()
    local = pltpu.make_async_copy(in_ref.at[sp], out_ref.at[sp], local_sem)
    local.start()
    for step in range(1, devices):
        copy(step, sp).wait_send()
        copy(step, (sp + devices - step) % devices).wait_recv()
    local.wait()


def exchange(blocks, identity):
    devices = blocks.shape[0]
    return pl.pallas_call(
        functools.partial(exchange_kernel, devices),
        out_shape=jax.ShapeDtypeStruct(blocks.shape, blocks.dtype),
        in_specs=[pl.BlockSpec(memory_space=pltpu.VMEM)],
        out_specs=pl.BlockSpec(memory_space=pltpu.VMEM),
        scratch_shapes=[
            pltpu.SemaphoreType.DMA((devices - 1,)),
            pltpu.SemaphoreType.DMA((devices - 1,)),
            pltpu.SemaphoreType.DMA,
        ],
        compiler_params=pltpu.CompilerParams(collective_id=identity, has_side_effects=True),
    )(blocks)


def gather_project(own, tail, span, sequence, width):
    sp, dp = lax.axis_size("sp"), lax.axis_size("dp")
    rows, columns = own.shape
    if 2 * rows % 128 or width % TILE:
        full, halo, spans = gather_rows(own, tail, span)
        halo = jnp.where(lax.axis_index("sp") > 0, halo, jnp.zeros_like(halo))
        extended = jnp.concatenate([halo, sequence], axis=0)
        return project(extended, full[:, :width]), full[:, width:], spans
    across = 1
    while 4 * across * across <= sp:
        across *= 2
    lines = (sp // across, across, dp // 2, 2)
    chips = sp * dp // 2
    length, model = sequence.shape
    lead = tail.shape[0]
    vmem = pl.BlockSpec(memory_space=pltpu.VMEM)
    projected, outw, spans = pl.pallas_call(
        functools.partial(gather_kernel, lines),
        out_shape=(
            jax.ShapeDtypeStruct((lead + length, width), own.dtype),
            jax.ShapeDtypeStruct((sp * dp, 2, rows // 2, columns - width), own.dtype),
            jax.ShapeDtypeStruct((sp,) + span.shape, span.dtype),
        ),
        in_specs=[vmem] * 4,
        out_specs=(vmem, pl.BlockSpec(memory_space=pl.ANY), vmem),
        scratch_shapes=[
            pltpu.VMEM((sp * dp, 2, rows // 2, columns), own.dtype),
            pltpu.VMEM(tail.shape, tail.dtype),
            pltpu.VMEM((lead + length, model), sequence.dtype),
            pltpu.VMEM((lead + length, width), jnp.float32),
            pltpu.SemaphoreType.DMA((chips,)),
            pltpu.SemaphoreType.DMA((2 * chips * 7,)),
            pltpu.SemaphoreType.DMA((chips, 2)),
            pltpu.SemaphoreType.DMA((chips, 2)),
            pltpu.SemaphoreType.DMA,
            pltpu.SemaphoreType.DMA((3,)),
            pltpu.SemaphoreType.DMA((sp - 1,)),
            pltpu.SemaphoreType.DMA((sp - 1,)),
        ],
        compiler_params=pltpu.CompilerParams(collective_id=1, has_side_effects=True),
    )(own.reshape(2, rows // 2, columns), tail, span, sequence)
    return projected, outw.reshape(sp * dp * rows, columns - width), spans


def gather_rows(own, tail, span):
    sp, dp = lax.axis_size("sp"), lax.axis_size("dp")
    across = 1
    while 4 * across * across <= sp:
        across *= 2
    lines = (sp // across, across, dp // 2, 2)
    chips = sp * dp // 2
    rows, columns = own.shape
    hops = 2 * chips * 7
    full, halo, spans = pl.pallas_call(
        functools.partial(gather_kernel, lines),
        out_shape=(
            jax.ShapeDtypeStruct((sp * dp, 2, rows // 2, columns), own.dtype),
            jax.ShapeDtypeStruct(tail.shape, tail.dtype),
            jax.ShapeDtypeStruct((sp,) + span.shape, span.dtype),
        ),
        in_specs=[pl.BlockSpec(memory_space=pltpu.VMEM)] * 3,
        out_specs=(
            pl.BlockSpec(memory_space=pl.ANY),
            pl.BlockSpec(memory_space=pltpu.VMEM),
            pl.BlockSpec(memory_space=pltpu.VMEM),
        ),
        scratch_shapes=[
            pltpu.SemaphoreType.DMA((hops,)),
            pltpu.SemaphoreType.DMA((chips, 2)),
            pltpu.SemaphoreType.DMA((chips, 2)),
            pltpu.SemaphoreType.DMA,
            pltpu.SemaphoreType.DMA((3,)),
            pltpu.SemaphoreType.DMA((sp - 1,)),
            pltpu.SemaphoreType.DMA((sp - 1,)),
        ],
        compiler_params=pltpu.CompilerParams(collective_id=1, has_side_effects=True),
    )(own.reshape(2, rows // 2, columns), tail, span)
    return full.reshape(sp * dp * rows, columns), halo, spans


def project(rows, weight):
    return jnp.dot(rows, weight, preferred_element_type=jnp.float32).astype(jnp.bfloat16)


def halo_conv(series, kernel, length):
    extent = kernel.shape[0]
    lead = series.shape[0] - length
    padded = series.astype(jnp.float32)
    taps = kernel.astype(jnp.float32)
    result = jnp.zeros((length, series.shape[1]), jnp.float32)
    for offset in range(extent):
        first = lead - extent + 1 + offset
        result = result + taps[offset] * padded[first : first + length]
    return jax.nn.silu(result).astype(jnp.bfloat16)


def exact(equation, left, right):
    return jnp.einsum(equation, left, right, precision=lax.Precision.HIGHEST)


def local_mix(values, inputs, reads, rates, decay):
    length = values.shape[0]
    blocks = length // BLOCK
    share = HEADS // GROUPS
    block_values = values.reshape(blocks, BLOCK, GROUPS, share, HEAD_DIM)
    block_inputs = inputs.reshape(blocks, BLOCK, GROUPS, STATE)
    block_reads = reads.reshape(blocks, BLOCK, GROUPS, STATE)
    block_rates = rates.reshape(blocks, BLOCK, HEADS)
    causal = jnp.tril(jnp.ones((BLOCK, BLOCK), dtype=bool))
    running = exact("ts,bsh->bth", causal.astype(jnp.float32), block_rates * decay)
    by_head = jnp.transpose(running, (0, 2, 1))
    rate_head = jnp.transpose(block_rates, (0, 2, 1))
    intervals = by_head[:, :, :, None] - by_head[:, :, None, :]
    fading = jnp.where(causal, jnp.exp(jnp.minimum(intervals, 0.0)), 0.0)
    fading = fading * rate_head[:, :, None, :]
    intersect = jnp.einsum(
        "btgn,bsgn->bgts", block_reads, block_inputs, preferred_element_type=jnp.float32
    )
    fading = fading.reshape(blocks, GROUPS, share, BLOCK, BLOCK)
    scores = (intersect[:, :, None] * fading).astype(jnp.bfloat16)
    within = jnp.einsum(
        "bgkts,bsgkp->btgkp", scores, block_values, preferred_element_type=jnp.float32
    )
    tail_fade = jnp.exp(running[:, -1:, :] - running) * block_rates
    tail_fade = tail_fade.reshape(blocks, BLOCK, GROUPS, share)
    weighted = (block_values.astype(jnp.float32) * tail_fade[..., None]).astype(jnp.bfloat16)
    states = jnp.einsum(
        "bsgkp,bsgn->bgkpn", weighted, block_inputs, preferred_element_type=jnp.float32
    )
    return within, states, running, block_reads


def entering_states(states, running, spans):
    blocks = states.shape[0]
    share = HEADS // GROUPS
    ends = running[:, -1, :]
    totals = jnp.cumsum(ends, axis=0)
    starts = totals - ends
    left = jnp.exp(totals[-1][None] - totals).reshape(blocks, GROUPS, share)
    last = jnp.sum(left[..., None, None] * states, axis=0)
    devices = lax.axis_size("sp")
    held = HEADS // devices
    came = exchange(last.astype(jnp.bfloat16).reshape(devices, held, HEAD_DIM, STATE), 2)
    own_spans = lax.dynamic_slice_in_dim(spans, lax.axis_index("sp") * held, held, 1)
    fades = jnp.exp(own_spans)[:, :, None, None]
    reached = jnp.zeros(came.shape[1:], jnp.float32)
    leaving = []
    for device in range(devices):
        leaving.append(reached.astype(jnp.bfloat16))
        reached = reached * fades[device] + came[device].astype(jnp.float32)
    initial = exchange(jnp.stack(leaving), 3).astype(jnp.float32)
    initial = initial.reshape(GROUPS, share, HEAD_DIM, STATE)
    current = initial
    entering = []
    for block in range(blocks):
        entering.append(current)
        fade = jnp.exp(ends[block]).reshape(GROUPS, share, 1, 1)
        current = current * fade + states[block]
    return jnp.stack(entering)


def per_device(
    activations,
    value_weight,
    gate_weight,
    input_weight,
    readout_weight,
    rate_weight,
    value_taps,
    input_taps,
    readout_taps,
    rate_bias,
    decay_log,
    norm_gain,
    out_weight,
):
    sequence = activations[0]
    length = sequence.shape[0]
    devices = lax.axis_size("sp")

    own = jnp.concatenate(
        [value_weight, input_weight, readout_weight, gate_weight, out_weight.T], axis=1
    )
    rate_raw = project(sequence, rate_weight)
    rates = jax.nn.softplus(rate_raw.astype(jnp.float32) + rate_bias)
    decay = -jnp.exp(decay_log) / (length * devices)
    span = jnp.zeros((8, 128), jnp.float32).at[:, :HEADS].set(jnp.sum(rates * decay, axis=0))
    ends = [0]
    for weight in (value_weight, input_weight, readout_weight, gate_weight):
        ends.append(ends[-1] + weight.shape[1])
    lead = 16
    projected, out_full, spans = gather_project(own, sequence[-lead:], span, sequence, ends[4])
    spans = spans[:, 0, :HEADS]
    values = halo_conv(projected[:, ends[0] : ends[1]], value_taps, length)
    inputs = halo_conv(projected[:, ends[1] : ends[2]], input_taps, length)
    reads = halo_conv(projected[:, ends[2] : ends[3]], readout_taps, length)
    within, states, running, block_reads = local_mix(values, inputs, reads, rates, decay)
    entering = entering_states(states, running, spans).astype(jnp.bfloat16)
    across = jnp.einsum(
        "btgn,bgkpn->btgkp", block_reads, entering, preferred_element_type=jnp.float32
    )
    fade = jnp.exp(running).reshape(across.shape[:4])
    mixed = (within + across * fade[..., None]).reshape(length, HEADS * HEAD_DIM)
    mixed = mixed.astype(jnp.bfloat16)
    gate_proj = projected[lead:, ends[3] : ends[4]]
    gated = mixed.astype(jnp.float32) * jax.nn.silu(gate_proj.astype(jnp.float32))
    scale = lax.rsqrt(jnp.mean(gated * gated, axis=-1, keepdims=True) + norm_eps)
    normed = (gated * scale * norm_gain).astype(jnp.bfloat16)
    result = lax.dot_general(
        normed, out_full, (((1,), (1,)), ((), ())), preferred_element_type=jnp.float32
    )
    return result.astype(jnp.bfloat16)[None]


def solution(mesh):
    placed = (
        P("dp", "sp", None),
        P(("sp", "dp"), None),
        P(("sp", "dp"), None),
        P(("sp", "dp"), None),
        P(("sp", "dp"), None),
        P(),
        P(),
        P(),
        P(),
        P(),
        P(),
        P(),
        P(None, ("sp", "dp")),
    )
    return jax.shard_map(
        per_device, mesh=mesh, in_specs=placed, out_specs=P("dp", "sp", None), check_vma=False
    )
```

```python
import functools
import itertools

import jax
import jax.numpy as jnp
from jax import lax
from jax.experimental import pallas as pl
from jax.experimental.pallas import tpu as pltpu
from jax.sharding import PartitionSpec as P

HEADS = 16
HEAD_DIM = 64
GROUPS = 4
STATE = 128
BLOCK = 128
LAG = 2
TILE = 512


norm_eps = 1.0


def nearest(count, place, rank):
    found = 0
    for start in range(count):
        order = sorted(range(count), key=lambda other: (abs(other - start), other))
        found = found + jnp.where(place == start, order[rank], 0)
    return found


def onward(count, place, origin, rank):
    if count == 2:
        return [(1 - place, None)] if rank == 0 else []
    steps = [1, -1] if rank == 0 else [jnp.where(origin < place, 1, -1)]
    pairs = []
    for step in steps:
        target = place + step
        pairs.append((target, jnp.logical_and(target >= 0, target < count)))
    return [pair for pair in pairs if count > 1]


def when(exists, action):
    if exists is None:
        action()
    else:
        pl.when(exists)(action)


def gather_kernel(
    lines,
    own_ref,
    tail_ref,
    span_ref,
    *rest,
):
    fused = len(rest) > 10
    if fused:
        seq_ref, proj_ref, outw_ref, spans_ref = rest[:4]
        full_ref, halo_ref, ext_ref, acc_ref, out_sem = rest[4:9]
    else:
        full_ref, halo_ref, spans_ref = rest[:3]
    (
        send_sem,
        recv_sem,
        pair_sem,
        local_sem,
        halo_sem,
        span_send,
        span_recv,
    ) = rest[-7:]
    depth, across, along, cores = lines
    sp = lax.axis_index("sp")
    dp = lax.axis_index("dp")
    here = (sp // across, sp % across, dp // cores)
    core = dp % cores
    counts = (depth, across, along)

    def target_id(place, which):
        return {"sp": place[0] * across + place[1], "dp": place[2] * cores + which}

    def moved(dim, value):
        return tuple(value if d == dim else here[d] for d in range(3))

    barrier = pltpu.get_barrier_semaphore()
    devices = depth * across
    peers = devices
    for step in range(1, devices):
        pl.semaphore_signal(
            barrier,
            inc=1,
            device_id={"sp": (sp + step) % devices, "dp": dp},
            device_id_type=pl.DeviceIdType.MESH,
        )
    for target, exists in onward(along, here[2], here[2], 0):

        def greet(target=target):
            pl.semaphore_signal(
                barrier,
                inc=1,
                device_id=target_id(moved(2, target), core),
                device_id_type=pl.DeviceIdType.MESH,
            )

        when(exists, greet)
        peers = peers + (1 if exists is None else jnp.where(exists, 1, 0))
    pl.semaphore_signal(
        barrier,
        inc=1,
        device_id=target_id(here, 1 - core),
        device_id_type=pl.DeviceIdType.MESH,
    )
    pl.semaphore_wait(barrier, peers)

    halo_copy = pltpu.make_async_remote_copy(
        src_ref=tail_ref,
        dst_ref=halo_ref,
        send_sem=halo_sem.at[0],
        recv_sem=halo_sem.at[1],
        device_id={"sp": (sp + 1) % devices, "dp": dp},
        device_id_type=pl.DeviceIdType.MESH,
    )
    pl.when(sp + 1 < devices)(halo_copy.start)
    own_span = pltpu.make_async_copy(span_ref, spans_ref.at[sp], halo_sem.at[2])
    own_span.start()

    def span_copy(step, slot):
        return pltpu.make_async_remote_copy(
            src_ref=span_ref,
            dst_ref=spans_ref.at[slot],
            send_sem=span_send.at[step - 1],
            recv_sem=span_recv.at[step - 1],
            device_id={"sp": (sp + step) % devices, "dp": dp},
            device_id_type=pl.DeviceIdType.MESH,
        )

    for step in range(1, devices):
        span_copy(step, sp).start()

    def chip_of(place):
        return (place[0] * across + place[1]) * along + place[2]

    mine = chip_of(here) * cores + core
    local = pltpu.make_async_copy(own_ref, full_ref.at[mine], local_sem)
    local.start()
    ranks = sorted(itertools.product(*(range(n) for n in counts)), key=lambda r: (sum(r), r))
    used = 0
    started = []
    chips = []

    def wait_pair(chip):
        for half in range(2):
            landed = full_ref.at[chip * cores + 1 - core, half]
            pltpu.make_async_remote_copy(
                src_ref=landed,
                dst_ref=landed,
                send_sem=send_sem.at[0],
                recv_sem=pair_sem.at[chip, half],
                device_id=target_id(here, 1 - core),
                device_id_type=pl.DeviceIdType.MESH,
            ).wait_recv()

    def out_copy(chip):
        width = proj_ref.shape[1]
        return pltpu.make_async_copy(
            full_ref.at[pl.ds(chip * cores, cores), :, :, pl.ds(width, outw_ref.shape[3])],
            outw_ref.at[pl.ds(chip * cores, cores)],
            out_sem.at[chip],
        )

    def accumulate(event):
        chip = chips[event]
        if event == 0:
            local.wait()
            lead = halo_ref.shape[0]

            def take():
                halo_copy.wait_recv()
                ext_ref[:lead] = halo_ref[...]

            def clear():
                ext_ref[:lead] = jnp.zeros_like(halo_ref)

            pl.when(sp > 0)(take)
            pl.when(sp == 0)(clear)
        wait_pair(chip)
        out_copy(chip).start()
        depth_rows = cores * 2 * full_ref.shape[2]
        rows = ext_ref[:, pl.ds(pl.multiple_of(chip * depth_rows, 128), depth_rows)]

        def tile(index, carry):
            columns = pl.ds(pl.multiple_of(index * TILE, TILE), TILE)
            piece = full_ref[pl.ds(chip * cores, cores), :, :, columns].reshape(depth_rows, TILE)
            product = jnp.dot(rows, piece, preferred_element_type=jnp.float32)
            if event == 0:
                acc_ref[:, columns] = product
            elif event == len(ranks) - 1:
                proj_ref[:, columns] = (acc_ref[:, columns] + product).astype(proj_ref.dtype)
            else:
                acc_ref[:, columns] += product
            return carry

        lax.fori_loop(0, proj_ref.shape[1] // TILE, tile, 0)

    for rank in ranks:
        origin = tuple(nearest(counts[d], here[d], rank[d]) for d in range(3))
        chip = chip_of(origin)
        block = chip * cores + core
        for half in range(2):
            landed = full_ref.at[block, half]
            source = own_ref.at[half] if sum(rank) == 0 else landed
            if sum(rank):
                pltpu.make_async_remote_copy(
                    src_ref=landed,
                    dst_ref=landed,
                    send_sem=send_sem.at[0],
                    recv_sem=recv_sem.at[chip, half],
                    device_id=target_id(here, 1 - core),
                    device_id_type=pl.DeviceIdType.MESH,
                ).wait_recv()
            order = (0, 1, 2) if half == 0 else (0, 2, 1)
            hops = []
            for position in (2, 1, 0):
                if any(rank[order[later]] for later in range(position + 1, 3)):
                    continue
                dim = order[position]
                for target, exists in onward(counts[dim], here[dim], origin[dim], rank[dim]):
                    hops.append((target_id(moved(dim, target), core), recv_sem, exists))
            hops.append((target_id(here, 1 - core), pair_sem, None))
            for device, sem, exists in hops:
                copy = pltpu.make_async_remote_copy(
                    src_ref=source,
                    dst_ref=landed,
                    send_sem=send_sem.at[used],
                    recv_sem=sem.at[chip, half],
                    device_id=device,
                    device_id_type=pl.DeviceIdType.MESH,
                )
                used += 1
                when(exists, copy.start)
                started.append((copy, exists))
        chips.append(chip)
        if fused and len(chips) == 1:
            ext_ref[halo_ref.shape[0] :] = seq_ref[...]
        if fused and len(chips) > LAG:
            accumulate(len(chips) - 1 - LAG)
    if fused:
        for event in range(len(chips) - LAG, len(chips)):
            accumulate(event)
    for copy, exists in started:
        when(exists, copy.wait_send)
    for chip in range(depth * across * along):
        if fused:
            out_copy(chip).wait()
        else:
            wait_pair(chip)
    if not fused:
        local.wait()
        pl.when(sp > 0)(halo_copy.wait_recv)
    own_span.wait()
    for step in range(1, devices):
        span_copy(step, sp).wait_send()
        span_copy(step, (sp + devices - step) % devices).wait_recv()
    pl.when(sp + 1 < devices)(halo_copy.wait_send)


def scan_kernel(
    devices, in_ref, fade_ref, out_ref, came_ref, leave_ref, send_sem, recv_sem, local_sem
):
    sp = lax.axis_index("sp")
    dp = lax.axis_index("dp")
    barrier = pltpu.get_barrier_semaphore()
    for step in range(1, devices):
        pl.semaphore_signal(
            barrier,
            inc=1,
            device_id={"sp": (sp + step) % devices, "dp": dp},
            device_id_type=pl.DeviceIdType.MESH,
        )
    pl.semaphore_wait(barrier, devices - 1)

    def exchange(phase, from_ref, to_ref):
        def copy(step, slot):
            target = (sp + step) % devices
            return pltpu.make_async_remote_copy(
                src_ref=from_ref.at[target],
                dst_ref=to_ref.at[slot],
                send_sem=send_sem.at[phase, step - 1],
                recv_sem=recv_sem.at[phase, step - 1],
                device_id={"sp": target, "dp": dp},
                device_id_type=pl.DeviceIdType.MESH,
            )

        for step in range(1, devices):
            copy(step, sp).start()
        local = pltpu.make_async_copy(from_ref.at[sp], to_ref.at[sp], local_sem.at[phase])
        local.start()
        for step in range(1, devices):
            copy(step, sp).wait_send()
            copy(step, (sp + devices - step) % devices).wait_recv()
        local.wait()

    exchange(0, in_ref, came_ref)
    reached = jnp.zeros(came_ref.shape[1:], jnp.float32)
    for device in range(devices):
        leave_ref[device] = reached.astype(leave_ref.dtype)
        reached = reached * fade_ref[device] + came_ref[device].astype(jnp.float32)
    exchange(1, leave_ref, out_ref)


def scan_states(blocks, fades):
    devices = blocks.shape[0]
    return pl.pallas_call(
        functools.partial(scan_kernel, devices),
        out_shape=jax.ShapeDtypeStruct(blocks.shape, blocks.dtype),
        in_specs=[pl.BlockSpec(memory_space=pltpu.VMEM)] * 2,
        out_specs=pl.BlockSpec(memory_space=pltpu.VMEM),
        scratch_shapes=[
            pltpu.VMEM(blocks.shape, blocks.dtype),
            pltpu.VMEM(blocks.shape, blocks.dtype),
            pltpu.SemaphoreType.DMA((2, devices - 1)),
            pltpu.SemaphoreType.DMA((2, devices - 1)),
            pltpu.SemaphoreType.DMA((2,)),
        ],
        compiler_params=pltpu.CompilerParams(collective_id=2, has_side_effects=True),
    )(blocks, fades)


def gather_project(own, tail, span, sequence, width):
    sp, dp = lax.axis_size("sp"), lax.axis_size("dp")
    rows, columns = own.shape
    if 2 * rows % 128 or width % TILE:
        full, halo, spans = gather_rows(own, tail, span)
        halo = jnp.where(lax.axis_index("sp") > 0, halo, jnp.zeros_like(halo))
        extended = jnp.concatenate([halo, sequence], axis=0)
        return project(extended, full[:, :width]), full[:, width:], spans
    across = 1
    while 4 * across * across <= sp:
        across *= 2
    lines = (sp // across, across, dp // 2, 2)
    chips = sp * dp // 2
    length, model = sequence.shape
    lead = tail.shape[0]
    vmem = pl.BlockSpec(memory_space=pltpu.VMEM)
    projected, outw, spans = pl.pallas_call(
        functools.partial(gather_kernel, lines),
        out_shape=(
            jax.ShapeDtypeStruct((lead + length, width), own.dtype),
            jax.ShapeDtypeStruct((sp * dp, 2, rows // 2, columns - width), own.dtype),
            jax.ShapeDtypeStruct((sp,) + span.shape, span.dtype),
        ),
        in_specs=[vmem] * 4,
        out_specs=(vmem, pl.BlockSpec(memory_space=pl.ANY), vmem),
        scratch_shapes=[
            pltpu.VMEM((sp * dp, 2, rows // 2, columns), own.dtype),
            pltpu.VMEM(tail.shape, tail.dtype),
            pltpu.VMEM((lead + length, model), sequence.dtype),
            pltpu.VMEM((lead + length, width), jnp.float32),
            pltpu.SemaphoreType.DMA((chips,)),
            pltpu.SemaphoreType.DMA((2 * chips * 7,)),
            pltpu.SemaphoreType.DMA((chips, 2)),
            pltpu.SemaphoreType.DMA((chips, 2)),
            pltpu.SemaphoreType.DMA,
            pltpu.SemaphoreType.DMA((3,)),
            pltpu.SemaphoreType.DMA((sp - 1,)),
            pltpu.SemaphoreType.DMA((sp - 1,)),
        ],
        compiler_params=pltpu.CompilerParams(collective_id=1, has_side_effects=True),
    )(own.reshape(2, rows // 2, columns), tail, span, sequence)
    return projected, outw.reshape(sp * dp * rows, columns - width), spans


def gather_rows(own, tail, span):
    sp, dp = lax.axis_size("sp"), lax.axis_size("dp")
    across = 1
    while 4 * across * across <= sp:
        across *= 2
    lines = (sp // across, across, dp // 2, 2)
    chips = sp * dp // 2
    rows, columns = own.shape
    hops = 2 * chips * 7
    full, halo, spans = pl.pallas_call(
        functools.partial(gather_kernel, lines),
        out_shape=(
            jax.ShapeDtypeStruct((sp * dp, 2, rows // 2, columns), own.dtype),
            jax.ShapeDtypeStruct(tail.shape, tail.dtype),
            jax.ShapeDtypeStruct((sp,) + span.shape, span.dtype),
        ),
        in_specs=[pl.BlockSpec(memory_space=pltpu.VMEM)] * 3,
        out_specs=(
            pl.BlockSpec(memory_space=pl.ANY),
            pl.BlockSpec(memory_space=pltpu.VMEM),
            pl.BlockSpec(memory_space=pltpu.VMEM),
        ),
        scratch_shapes=[
            pltpu.SemaphoreType.DMA((hops,)),
            pltpu.SemaphoreType.DMA((chips, 2)),
            pltpu.SemaphoreType.DMA((chips, 2)),
            pltpu.SemaphoreType.DMA,
            pltpu.SemaphoreType.DMA((3,)),
            pltpu.SemaphoreType.DMA((sp - 1,)),
            pltpu.SemaphoreType.DMA((sp - 1,)),
        ],
        compiler_params=pltpu.CompilerParams(collective_id=1, has_side_effects=True),
    )(own.reshape(2, rows // 2, columns), tail, span)
    return full.reshape(sp * dp * rows, columns), halo, spans


def project(rows, weight):
    return jnp.dot(rows, weight, preferred_element_type=jnp.float32).astype(jnp.bfloat16)


def halo_conv(series, kernel, length):
    extent = kernel.shape[0]
    lead = series.shape[0] - length
    padded = series.astype(jnp.float32)
    taps = kernel.astype(jnp.float32)
    result = jnp.zeros((length, series.shape[1]), jnp.float32)
    for offset in range(extent):
        first = lead - extent + 1 + offset
        result = result + taps[offset] * padded[first : first + length]
    return jax.nn.silu(result).astype(jnp.bfloat16)


def exact(equation, left, right):
    return jnp.einsum(equation, left, right, precision=lax.Precision.HIGHEST)


def local_mix(values, inputs, reads, rates, decay):
    length = values.shape[0]
    blocks = length // BLOCK
    share = HEADS // GROUPS
    block_values = values.reshape(blocks, BLOCK, GROUPS, share, HEAD_DIM)
    block_inputs = inputs.reshape(blocks, BLOCK, GROUPS, STATE)
    block_reads = reads.reshape(blocks, BLOCK, GROUPS, STATE)
    block_rates = rates.reshape(blocks, BLOCK, HEADS)
    causal = jnp.tril(jnp.ones((BLOCK, BLOCK), dtype=bool))
    running = exact("ts,bsh->bth", causal.astype(jnp.float32), block_rates * decay)
    by_head = jnp.transpose(running, (0, 2, 1))
    rate_head = jnp.transpose(block_rates, (0, 2, 1))
    intervals = by_head[:, :, :, None] - by_head[:, :, None, :]
    fading = jnp.where(causal, jnp.exp(jnp.minimum(intervals, 0.0)), 0.0)
    fading = fading * rate_head[:, :, None, :]
    intersect = jnp.einsum(
        "btgn,bsgn->bgts", block_reads, block_inputs, preferred_element_type=jnp.float32
    )
    fading = fading.reshape(blocks, GROUPS, share, BLOCK, BLOCK)
    scores = (intersect[:, :, None] * fading).astype(jnp.bfloat16)
    within = jnp.einsum(
        "bgkts,bsgkp->btgkp", scores, block_values, preferred_element_type=jnp.float32
    )
    tail_fade = jnp.exp(running[:, -1:, :] - running) * block_rates
    tail_fade = tail_fade.reshape(blocks, BLOCK, GROUPS, share)
    weighted = (block_values.astype(jnp.float32) * tail_fade[..., None]).astype(jnp.bfloat16)
    states = jnp.einsum(
        "bsgkp,bsgn->bgkpn", weighted, block_inputs, preferred_element_type=jnp.float32
    )
    return within, states, running, block_reads


def entering_states(states, running, spans):
    blocks = states.shape[0]
    share = HEADS // GROUPS
    ends = running[:, -1, :]
    totals = jnp.cumsum(ends, axis=0)
    starts = totals - ends
    left = jnp.exp(totals[-1][None] - totals).reshape(blocks, GROUPS, share)
    last = jnp.sum(left[..., None, None] * states, axis=0)
    devices = lax.axis_size("sp")
    held = HEADS // devices
    own_spans = lax.dynamic_slice_in_dim(spans, lax.axis_index("sp") * held, held, 1)
    fades = jnp.broadcast_to(jnp.exp(own_spans)[:, :, None, None], (devices, held, 1, STATE))
    packed = last.astype(jnp.bfloat16).reshape(devices, held, HEAD_DIM, STATE)
    initial = scan_states(packed, fades).astype(jnp.float32)
    initial = initial.reshape(GROUPS, share, HEAD_DIM, STATE)
    current = initial
    entering = []
    for block in range(blocks):
        entering.append(current)
        fade = jnp.exp(ends[block]).reshape(GROUPS, share, 1, 1)
        current = current * fade + states[block]
    return jnp.stack(entering)


def per_device(
    activations,
    value_weight,
    gate_weight,
    input_weight,
    readout_weight,
    rate_weight,
    value_taps,
    input_taps,
    readout_taps,
    rate_bias,
    decay_log,
    norm_gain,
    out_weight,
):
    sequence = activations[0]
    length = sequence.shape[0]
    devices = lax.axis_size("sp")

    own = jnp.concatenate(
        [value_weight, input_weight, readout_weight, gate_weight, out_weight.T], axis=1
    )
    rate_raw = project(sequence, rate_weight)
    rates = jax.nn.softplus(rate_raw.astype(jnp.float32) + rate_bias)
    decay = -jnp.exp(decay_log) / (length * devices)
    span = jnp.zeros((8, 128), jnp.float32).at[:, :HEADS].set(jnp.sum(rates * decay, axis=0))
    ends = [0]
    for weight in (value_weight, input_weight, readout_weight, gate_weight):
        ends.append(ends[-1] + weight.shape[1])
    lead = 16
    projected, out_full, spans = gather_project(own, sequence[-lead:], span, sequence, ends[4])
    spans = spans[:, 0, :HEADS]
    values = halo_conv(projected[:, ends[0] : ends[1]], value_taps, length)
    inputs = halo_conv(projected[:, ends[1] : ends[2]], input_taps, length)
    reads = halo_conv(projected[:, ends[2] : ends[3]], readout_taps, length)
    within, states, running, block_reads = local_mix(values, inputs, reads, rates, decay)
    entering = entering_states(states, running, spans).astype(jnp.bfloat16)
    across = jnp.einsum(
        "btgn,bgkpn->btgkp", block_reads, entering, preferred_element_type=jnp.float32
    )
    fade = jnp.exp(running).reshape(across.shape[:4])
    mixed = (within + across * fade[..., None]).reshape(length, HEADS * HEAD_DIM)
    mixed = mixed.astype(jnp.bfloat16)
    gate_proj = projected[lead:, ends[3] : ends[4]]
    gated = mixed.astype(jnp.float32) * jax.nn.silu(gate_proj.astype(jnp.float32))
    scale = lax.rsqrt(jnp.mean(gated * gated, axis=-1, keepdims=True) + norm_eps)
    normed = (gated * scale * norm_gain).astype(jnp.bfloat16)
    result = lax.dot_general(
        normed, out_full, (((1,), (1,)), ((), ())), preferred_element_type=jnp.float32
    )
    return result.astype(jnp.bfloat16)[None]


def solution(mesh):
    placed = (
        P("dp", "sp", None),
        P(("sp", "dp"), None),
        P(("sp", "dp"), None),
        P(("sp", "dp"), None),
        P(("sp", "dp"), None),
        P(),
        P(),
        P(),
        P(),
        P(),
        P(),
        P(),
        P(None, ("sp", "dp")),
    )
    return jax.shard_map(
        per_device, mesh=mesh, in_specs=placed, out_specs=P("dp", "sp", None), check_vma=False
    )
```
